32 devices in a mesh: ep: 8 (over z, x), tp: 4 (over y, core).
Axes of the slice: x: 2, y: 2, z: 4, core: 2. Of those that a mesh axis runs over, the one named last changes fastest.
Arguments:
- recurrence_query: bfloat16 [1024, 1024], P('ep', 'tp'), may hold values from -6 to 6
- forget_preactivation: bfloat16 [1024, 1024], P('ep', 'tp'), may hold values from -7 to 7
- recurrence_value: bfloat16 [1024, 1024], P('ep', 'tp'), may hold values from -6 to 6
- output_gate_preactivation: bfloat16 [1024, 1024], P('ep', 'tp'), may hold values from -6 to 6
- forget_margin: float32 [1024], P('tp'), may hold values from 0 to 0.1
- surge_log_decay: float32 [8, 1024], P('tp', 'ep'), may hold values from -1.4 to 0
- head_norm_gain: float32 [1024], P('tp'), may hold values from 0.1 to 1.9
- recurrence_output_matrix: bfloat16 [1024, 4096], P('tp'), may hold values from -0.1875 to 0.1875
- second_micro_input: bfloat16 [1024, 4096], P(('ep', 'tp')), may hold values from -6 to 6
- expert_norm_gain: float32 [4096], replicated, may hold values from 0.1 to 1.9
- routes: int32 [1024, 2], P('ep'), may hold values from 0 to 7, all different within a row; in each aligned block of 32 rows (0 to 31, 32 to 63, ...) at most 16 rows name the same one
- router_chosen_logits: float32 [1024, 2], P(('ep', 'tp')), may hold values from -6 to 6
- expert_gate_matrix: bfloat16 [8, 4096, 1408], P('ep', None, 'tp'), may hold values from -0.09375 to 0.09375
- expert_up_matrix: bfloat16 [8, 4096, 1408], P('ep', None, 'tp'), may hold values from -0.09375 to 0.09375
- expert_down_matrix: bfloat16 [8, 1408, 4096], P('ep', 'tp'), may hold values from -0.15625 to 0.15625
Outputs:
- mixed: bfloat16 [1024, 4096], P(('ep', 'tp'))
- moe_out: bfloat16 [1024, 4096], P(('ep', 'tp'))
The draws below stay inside these ranges and needn't reach their ends.
Inputs may be any that keep to these rules, and one draw needn't show every extreme that they name: `routes`: in the rows of one device (aligned blocks of 32 rows) no expert is named more than 16 times, and the experts of a row differ.
All inputs are finite; a program needn't handle non-finite values.
Results may differ from the reference program's by a relative error of at most 0.019.
Values may be sent and summed in bfloat16 or wider, within the bound.
A program may use at most 128 MiB of HBM per device.

```python
import math
import jax
import jax.numpy as jnp
import numpy as np
from jax import lax

D = 4096
HEADS = 8
KEY = 128
VAL = 128
FF = 1408
TOP = 2
SPAN = 64
SEQ_DEV = 128
TB_DEV = 32
EXPERTS = 8
CAP = 16
TOKENS_A = 1024
TOKENS_B = 1024
N_EP = 8
N_TP = 4


def draw_forget_preactivation(key, part):
    noise_key, shift_key = jax.random.split(jax.random.fold_in(key, 11))
    blocks = TOKENS_A // SEQ_DEV
    shifts = jax.random.uniform(shift_key, (blocks, 1, HEADS * KEY), jnp.float32, -1.0, 1.0)
    noise = jnp.clip(jax.random.normal(noise_key, (blocks, SEQ_DEV, HEADS * KEY), jnp.float32), -6.0, 6.0)
    return (noise + shifts).reshape(TOKENS_A, HEADS * KEY).astype(jnp.bfloat16)


def draw_forget_margin(key, part):
    pick_key, fast_key, slow_key = jax.random.split(jax.random.fold_in(key, 23), 3)
    share = 0.5
    fast_head = jax.random.uniform(pick_key, (HEADS, 1), jnp.float32) < share
    fast_gap = jnp.exp(jax.random.uniform(fast_key, (HEADS, KEY), jnp.float32, math.log(0.04), math.log(0.1)))
    slow_gap = jnp.exp(jax.random.uniform(slow_key, (HEADS, KEY), jnp.float32, math.log(0.3), math.log(1.5))) / TOKENS_A
    return jnp.where(fast_head, fast_gap, slow_gap).reshape(HEADS * KEY).astype(jnp.float32)


def draw_surge_log_decay(key, part):
    spot_key, depth_key = jax.random.split(jax.random.fold_in(key, 37))
    spots = jax.random.randint(spot_key, (HEADS, 2, 1), 0, TOKENS_A)
    depth = jax.random.uniform(depth_key, (HEADS, 2, 1), jnp.float32, math.log(0.5), math.log(0.8))
    hits = spots == jnp.arange(TOKENS_A, dtype=jnp.int32)[None, None, :]
    return jnp.sum(jnp.where(hits, depth, 0.0), axis=1).astype(jnp.float32)


def block_levels(stream_key, extent, shards, low, high):
    level, own = 1.0, jax.random.fold_in(stream_key, 6)
    for axis_at, parts in shards:
        heights = jnp.exp(jax.random.uniform(jax.random.fold_in(own, axis_at), (parts,), jnp.float32, low / len(shards), high / len(shards)))
        level = level * jnp.repeat(heights, extent[axis_at] // parts).reshape([-1 if axis == axis_at else 1 for axis in range(len(extent))])
    return level


def deal_out(own_key, own, number, rows, amount, top, most, slope):
    order = jax.random.permutation(own_key, amount)
    heavy_load, ordinary = shares(amount, rows * top, most, slope, True), shares(amount, rows * top, most, slope, False)
    places = jnp.arange(amount)

    def named(tallies, turn):
        used = int((tallies > 0).sum())
        fixed = max(1, used // 4)
        passed = fixed + (places - fixed + turn * (used - fixed)) % max(1, amount - fixed)
        return jnp.zeros((amount,), jnp.int32).at[order[jnp.where(places < fixed, places, passed)]].set(jnp.asarray(tallies, jnp.int32))

    tallies = jnp.where(number % 4 == 0, named(heavy_load, number // 4), named(ordinary, number - number // 4 - 1))
    mixed = jax.random.permutation(jax.random.fold_in(own, 3), amount)
    donor, taker = mixed[0:amount // 2 * 2:2], mixed[1:amount // 2 * 2:2]
    margin = jnp.minimum(tallies[donor] - 1, most - tallies[taker]) // 2
    margin = jnp.where((donor == order[0]) | (taker == order[0]) | (tallies[taker] == 0), 0, jnp.maximum(margin, 0))
    passed = jax.random.randint(jax.random.fold_in(own, 4), (amount // 2,), 0, 1 << 20) % (margin + 1)
    tallies = tallies.at[donor].add(-passed).at[taker].add(passed)
    items = jnp.searchsorted(jnp.cumsum(tallies), jnp.arange(rows * top), side="right").astype(jnp.int32)
    grid = items.reshape(top, rows).T
    grid = grid[jax.random.permutation(jax.random.fold_in(own, 1), rows)]
    turn = jax.random.randint(jax.random.fold_in(own, 2), (rows, 1), 0, top)
    return jnp.take_along_axis(grid, (jnp.arange(top)[None, :] + turn) % top, axis=1)


def shares(count, total, bound, slope, full):
    weights = [(1 << 20) // math.isqrt(grade ** slope) + 1 for grade in range(1, count + 1)]
    largest = bound if full else min(bound, max(-(-total // count), total * weights[0] // sum(weights)))
    least = 1 if total - largest >= count - 1 else 0
    holding, surplus = [largest] + [least] * (count - 1), total - largest - least * (count - 1)
    while surplus > 0:
        candidates = [i for i in range(1, count) if holding[i] < largest] or [i for i in range(1, count) if holding[i] < bound]
        whole, remaining = sum([weights[i] for i in candidates]), surplus
        for i in candidates:
            addition = min(bound - holding[i], max(1, remaining * weights[i] // whole), surplus)
            holding[i] = holding[i] + addition
            surplus = surplus - addition
    return np.array(holding)


def normal_values(rng, dims, deviation, reach, shards=(), kind=jnp.bfloat16):
    values = jax.random.normal(rng, dims, jnp.float32) * deviation
    if len(shards) > 0:
        values = block_levels(rng, dims, shards, -0.22, 0.18) * values
    return jnp.clip(values, min=-reach, max=reach).astype(kind)


def setup_inputs(seed: int = 0) -> dict:
    streams_of = jax.random.split(jax.random.key(seed), 16)
    recurrence_query = normal_values(streams_of[0], (TOKENS_A, HEADS * KEY), 1.0, 6.0, ((0, 8), (1, 4)))
    forget_preactivation = draw_forget_preactivation(jax.random.fold_in(streams_of[15], 71), 0)
    recurrence_value = normal_values(streams_of[2], (TOKENS_A, HEADS * VAL), 1.0, 6.0, ((0, 8), (1, 4)))
    output_gate_preactivation = normal_values(streams_of[3], (TOKENS_A, HEADS * VAL), 1.0, 6.0, ((0, 8), (1, 4)))
    forget_margin = draw_forget_margin(jax.random.fold_in(streams_of[15], 71), 0)
    surge_log_decay = draw_surge_log_decay(jax.random.fold_in(streams_of[15], 71), 0)
    head_norm_gain = jnp.clip(1.0 + 0.18 * jax.random.normal(streams_of[6], (HEADS * VAL,), jnp.float32), 0.1, 1.9)
    recurrence_output_matrix = normal_values(streams_of[7], (HEADS * VAL, D), (HEADS * VAL) ** -0.5, 0.1875, ((0, 4),))
    second_micro_input = normal_values(streams_of[8], (TOKENS_B, D), 1.0, 6.0, ((0, 32),))
    expert_norm_gain = jnp.clip(1.0 + 0.18 * jax.random.normal(streams_of[9], (D,), jnp.float32), 0.1, 1.9)
    routes_keys = jax.random.split(jax.random.fold_in(streams_of[10], 1), TOKENS_B // TB_DEV)
    routes_turns = jax.random.permutation(jax.random.fold_in(streams_of[10], 3), TOKENS_B // TB_DEV)
    routes = jax.vmap(lambda own, number: deal_out(jax.random.fold_in(streams_of[10], 2), own, number, TB_DEV, EXPERTS, TOP, CAP, 1))(routes_keys, routes_turns).reshape((TOKENS_B, TOP))
    router_chosen_logits = normal_values(streams_of[11], (TOKENS_B, TOP), 1.0, 6.0, ((0, 32),), jnp.float32)
    expert_gate_matrix = normal_values(streams_of[12], (EXPERTS, D, FF), D ** -0.5, 0.09375, ((0, 8), (2, 4)))
    expert_up_matrix = normal_values(streams_of[13], (EXPERTS, D, FF), D ** -0.5, 0.09375, ((0, 8), (2, 4)))
    expert_down_matrix = normal_values(streams_of[14], (EXPERTS, FF, D), FF ** -0.5, 0.15625, ((0, 8), (1, 4)))
    return {"recurrence_query": recurrence_query, "forget_preactivation": forget_preactivation, "recurrence_value": recurrence_value, "output_gate_preactivation": output_gate_preactivation, "forget_margin": forget_margin, "surge_log_decay": surge_log_decay, "head_norm_gain": head_norm_gain, "recurrence_output_matrix": recurrence_output_matrix, "second_micro_input": second_micro_input, "expert_norm_gain": expert_norm_gain, "routes": routes, "router_chosen_logits": router_chosen_logits, "expert_gate_matrix": expert_gate_matrix, "expert_up_matrix": expert_up_matrix, "expert_down_matrix": expert_down_matrix}


epsilon = 1e-06
highest = lax.Precision.HIGHEST

def span_recurrence(query, inflow, decay_logarithm, values):
    number_of_heads, seq_len, key_width = query.shape
    span_count = seq_len // SPAN

    def to_spans(array):
        return array.reshape(number_of_heads, span_count, SPAN, array.shape[-1]).transpose(1, 0, 2, 3)
    lower_mask = jnp.tril(jnp.ones((SPAN, SPAN), bool))

    def advance(carried, inputs):
        query_span, inflow_span, decay_span, value_span = inputs
        running = jnp.cumsum(decay_span, axis=1)
        lifted_query = query_span * jnp.exp(running)
        lowered_inflow = inflow_span * jnp.exp(-running)
        scores = jnp.einsum('htd,hsd->hts', lifted_query, lowered_inflow, precision=highest)
        scores = jnp.where(lower_mask[None, :, :], scores, 0.0)
        output = jnp.einsum('hts,hsv->htv', scores, value_span, precision=highest)
        output = output + jnp.einsum('htd,hdv->htv', lifted_query, carried, precision=highest)
        closing = running[:, -1:, :]
        updated = jnp.exp(closing[:, 0, :])[:, :, None] * carried + jnp.einsum('hsd,hsv->hdv', inflow_span * jnp.exp(closing - running), value_span, precision=highest)
        return (updated, output)
    start_state = jnp.zeros((number_of_heads, key_width, values.shape[-1]), jnp.float32)
    final_state, outputs = lax.scan(advance, start_state, (to_spans(query), to_spans(inflow), to_spans(decay_logarithm), to_spans(values)))
    return (final_state, outputs.transpose(1, 0, 2, 3).reshape(number_of_heads, seq_len, values.shape[-1]))

def split_sum(left, right, groups):
    group_width = left.shape[1] // groups
    total = jnp.zeros((left.shape[0], right.shape[1]), jnp.float32)
    for portion in range(groups):
        piece = jnp.dot(left[:, portion * group_width:(portion + 1) * group_width], right[portion * group_width:(portion + 1) * group_width], preferred_element_type=jnp.float32)
        rounded = lax.optimization_barrier(piece.astype(jnp.bfloat16))
        total = total + rounded.astype(jnp.float32)
    return total.astype(jnp.bfloat16)

def reference(recurrence_query, forget_preactivation, recurrence_value, output_gate_preactivation, forget_margin, surge_log_decay, head_norm_gain, recurrence_output_matrix, second_micro_input, expert_norm_gain, routes, router_chosen_logits, expert_gate_matrix, expert_up_matrix, expert_down_matrix):
    seq_len = recurrence_query.shape[0]

    def heads_leading(array):
        return array.astype(jnp.float32).reshape(seq_len, HEADS, -1).transpose(1, 0, 2)
    closed_flag = jax.nn.sigmoid(-forget_preactivation.astype(jnp.float32)) * forget_margin
    decay_logarithm = heads_leading(jnp.log1p(-closed_flag)) + surge_log_decay[:, :, None]
    query = heads_leading(recurrence_query)
    _, output = span_recurrence(query, heads_leading(closed_flag), decay_logarithm, heads_leading(recurrence_value))
    output = output * lax.rsqrt(lax.optimization_barrier(jnp.mean(output * output, axis=-1, keepdims=True)) + epsilon)
    output = output.transpose(1, 0, 2).reshape(seq_len, -1)
    hidden_a = (output * head_norm_gain * jax.nn.silu(output_gate_preactivation.astype(jnp.float32))).astype(jnp.bfloat16)
    mixed = split_sum(hidden_a, recurrence_output_matrix, N_TP)
    moe_rows = second_micro_input.astype(jnp.float32)
    normed = (moe_rows * lax.rsqrt(lax.optimization_barrier(jnp.mean(moe_rows * moe_rows, axis=-1, keepdims=True)) + epsilon) * expert_norm_gain).astype(jnp.bfloat16)
    flat_routes = routes.reshape(-1)
    copies = flat_routes.shape[0]
    max_rows = N_EP * N_TP * CAP

    def per_expert(written, expert_id):
        picked_order = jnp.argsort((flat_routes != expert_id).astype(jnp.int32), stable=True)[:max_rows]
        picked_order = picked_order.astype(jnp.int32)
        is_live = flat_routes[picked_order] == expert_id
        picked = normed[picked_order // TOP]
        gate_proj = jnp.dot(picked, expert_gate_matrix[expert_id], preferred_element_type=jnp.float32)
        up_proj = jnp.dot(picked, expert_up_matrix[expert_id], preferred_element_type=jnp.float32)
        hidden_b = (jax.nn.silu(gate_proj) * up_proj).astype(jnp.bfloat16)
        result = split_sum(hidden_b, expert_down_matrix[expert_id], N_TP)
        kept_rows = jnp.where(is_live[:, None], result, written[picked_order])
        return (written.at[picked_order].set(kept_rows), None)
    outputs, _ = lax.scan(per_expert, jnp.zeros((copies, D), jnp.bfloat16), jnp.arange(EXPERTS, dtype=jnp.int32))
    route_weight = jax.nn.softmax(router_chosen_logits.astype(jnp.float32), axis=-1)
    moe_out = lax.optimization_barrier(jnp.sum(route_weight[:, :, None] * outputs.reshape(-1, TOP, D).astype(jnp.float32), axis=1))
    return (mixed, moe_out.astype(jnp.bfloat16))
```

```python
import functools

import jax
import jax.numpy as jnp
from jax import lax
from jax.experimental import pallas as pl
from jax.experimental.pallas import tpu as pltpu
from jax.sharding import PartitionSpec as P

TOP = 2
SPAN = 64
MESH = pl.DeviceIdType.MESH


epsilon = 1e-06
highest = lax.Precision.HIGHEST


def visiting_order(count):
    return sorted(range(1, count), key=lambda k: abs(k - count // 2)) + [0]


def greet(me, tp, ep_count, tp_count):
    pairs = tp_count // 2
    pair, side = tp // 2, tp % 2
    barrier = pltpu.get_barrier_semaphore()
    for k in range(1, ep_count):
        pl.semaphore_signal(
            barrier,
            inc=1,
            device_id={"ep": lax.rem(me + k, ep_count), "tp": tp},
            device_id_type=MESH,
        )
    for j in range(1, pairs):
        pl.semaphore_signal(
            barrier,
            inc=1,
            device_id={"ep": me, "tp": lax.rem(pair + j, pairs) * 2 + side},
            device_id_type=MESH,
        )
    pl.semaphore_signal(
        barrier, inc=1, device_id={"ep": me, "tp": pair * 2 + 1 - side}, device_id_type=MESH
    )
    pl.semaphore_wait(barrier, ep_count + pairs - 1)


def dispatch_kernel(
    ep_count, tp_count, slots, state, piece, states, sa, ra, sy, ry, sc, rc, ss, rs
):
    me, tp = lax.axis_index("ep"), lax.axis_index("tp")
    pairs = tp_count // 2
    pair, side = tp // 2, tp % 2
    other = pair * 2 + 1 - side
    order = visiting_order(ep_count)

    def remote(src, dst, send, recv, ep, to):
        return pltpu.make_async_remote_copy(
            src_ref=src,
            dst_ref=dst,
            send_sem=send,
            recv_sem=recv,
            device_id={"ep": ep, "tp": to},
            device_id_type=MESH,
        )

    states[...] = jnp.zeros_like(states)
    greet(me, tp, ep_count, tp_count)

    def exchange(k):
        to = lax.rem(me + k, ep_count)
        return remote(slots.at[to], piece.at[tp, me], sa.at[k], ra.at[k], to, tp)

    def state_copy(k):
        to = lax.rem(me + k, ep_count)
        return remote(state, states.at[me], ss.at[k], rs.at[k], to, tp)

    for k in order[:-1]:
        exchange(k).start()

    def source(k):
        return lax.rem(me + ep_count - k, ep_count)

    def own_block(k):
        return slots.at[me] if k == 0 else piece.at[tp, source(k)]

    def across(k, j):
        to = lax.rem(pair + j, pairs) * 2 + side
        return remote(own_block(k), piece.at[tp, source(k)], sy.at[j, k], ry.at[j, k], me, to)

    def beside(k, j):
        block = lax.rem(pair + pairs - j, pairs) * 2 + side
        src = own_block(k) if j == 0 else piece.at[block, source(k)]
        return remote(src, piece.at[block, source(k)], sc.at[j, k], rc.at[j, k], me, other)

    def pass_on(k):
        for j in range(1, pairs):
            across(k, j).start()
        beside(k, 0).start()

    pass_on(0)
    for k in range(1, ep_count):

        @pl.when(me + k < ep_count)
        def _(k=k):
            state_copy(k).start()

    piece[tp, me] = slots[me]
    sequence = [0] + order[:-1]
    for position, k in enumerate(sequence):
        if k:
            exchange(k).wait_recv()
            pass_on(k)
        if position:
            before = sequence[position - 1]
            for j in range(1, pairs):
                across(before, j).wait_recv()
                beside(before, j).start()
    for j in range(1, pairs):
        across(sequence[-1], j).wait_recv()
        beside(sequence[-1], j).start()
    for k in range(1, ep_count):

        @pl.when(me + k < ep_count)
        def _(k=k):
            state_copy(k).wait_send()

        @pl.when(me - k >= 0)
        def _(k=k):
            state_copy(k).wait_recv()

        exchange(k).wait_send()
    for k in sequence:
        for j in range(pairs):
            if j:
                across(k, j).wait_send()
            beside(k, j).wait_send()
            beside(k, j).wait_recv()


def dispatch(slots, state, ep_count, tp_count):
    pairs = tp_count // 2
    dma = pltpu.SemaphoreType.DMA
    vmem = pl.BlockSpec(memory_space=pltpu.VMEM)
    return pl.pallas_call(
        functools.partial(dispatch_kernel, ep_count, tp_count),
        out_shape=(
            jax.ShapeDtypeStruct((tp_count,) + slots.shape, slots.dtype),
            jax.ShapeDtypeStruct((ep_count,) + state.shape, state.dtype),
        ),
        in_specs=[vmem] * 2,
        out_specs=(vmem, vmem),
        scratch_shapes=[
            dma((ep_count,)),
            dma((ep_count,)),
            dma((pairs, ep_count)),
            dma((pairs, ep_count)),
            dma((pairs, ep_count)),
            dma((pairs, ep_count)),
            dma((ep_count,)),
            dma((ep_count,)),
        ],
        compiler_params=pltpu.CompilerParams(collective_id=0, has_side_effects=True),
    )(slots, state)


def return_kernel(
    ep_count,
    tp_count,
    parts,
    mix,
    mixed,
    returned,
    cbuf,
    cmix,
    ysend,
    ysmix,
    ybuf,
    ymix,
    abuf,
    sc,
    rc,
    sy,
    ry,
    sa,
    ra,
):
    me, tp = lax.axis_index("ep"), lax.axis_index("tp")
    pairs = tp_count // 2
    pair, side = tp // 2, tp % 2
    other = pair * 2 + 1 - side
    order = visiting_order(ep_count)
    greet(me, tp, ep_count, tp_count)

    def remote(src, dst, send, recv, ep, to):
        return pltpu.make_async_remote_copy(
            src_ref=src,
            dst_ref=dst,
            send_sem=send,
            recv_sem=recv,
            device_id={"ep": ep, "tp": to},
            device_id_type=MESH,
        )

    def chunk(k):
        return lax.rem(me + k, ep_count)

    def toward(j):
        return lax.rem(pair + j, pairs)

    def beside(k, j):
        block = toward(j) * 2 + 1 - side
        if k == ep_count:
            return remote(mix.at[block], cmix.at[j], sc.at[j, k], rc.at[j, k], me, other)
        return remote(parts.at[block, chunk(k)], cbuf.at[j, k], sc.at[j, k], rc.at[j, k], me, other)

    def across(k, j):
        to = toward(j) * 2 + side
        if k == ep_count:
            return remote(ysmix.at[j], ymix.at[j], sy.at[j, k], ry.at[j, k], me, to)
        return remote(ysend.at[j, k], ybuf.at[j, k], sy.at[j, k], ry.at[j, k], me, to)

    def home(k):
        return remote(abuf.at[k], returned.at[me], sa.at[k], ra.at[k], chunk(k), tp)

    wide = jnp.float32
    everything = order + [ep_count]
    for k in everything:
        for j in list(range(1, pairs)) + [0]:
            beside(k, j).start()
    for k in everything:
        for j in range(1, pairs):
            beside(k, j).wait_recv()
            block = toward(j) * 2 + side
            if k == ep_count:
                ysmix[j] = (mix[block].astype(wide) + cmix[j].astype(wide)).astype(mix.dtype)
            else:
                ysend[j, k] = (
                    parts[block, chunk(k)].astype(wide) + cbuf[j, k].astype(wide)
                ).astype(parts.dtype)
            across(k, j).start()
    for k in everything:
        beside(k, 0).wait_recv()
        if k == ep_count:
            total = mix[tp].astype(wide) + cmix[0].astype(wide)
        else:
            total = parts[tp, chunk(k)].astype(wide) + cbuf[0, k].astype(wide)
        for j in range(1, pairs):
            across(k, j).wait_recv()
            total = total + (ymix[j] if k == ep_count else ybuf[j, k]).astype(wide)
        total = total.astype(parts.dtype)
        if k == ep_count:
            mixed[...] = total
        elif k == 0:
            returned[me] = total
        else:
            abuf[k] = total
            home(k).start()
    for k in everything:
        for j in range(pairs):
            beside(k, j).wait_send()
            if j:
                across(k, j).wait_send()
        if 0 < k < ep_count:
            home(k).wait()


def give_back(parts, mix, ep_count, tp_count):
    pairs = tp_count // 2
    dma = pltpu.SemaphoreType.DMA
    vmem = pl.BlockSpec(memory_space=pltpu.VMEM)
    chunks, rows = parts.shape[1:], mix.shape[1:]
    many = (pairs, ep_count + 1)
    kind = parts.dtype
    return pl.pallas_call(
        functools.partial(return_kernel, ep_count, tp_count),
        out_shape=(
            jax.ShapeDtypeStruct(rows, kind),
            jax.ShapeDtypeStruct(chunks, kind),
        ),
        in_specs=[vmem] * 2,
        out_specs=(vmem, vmem),
        scratch_shapes=[
            pltpu.VMEM((pairs,) + chunks, kind),
            pltpu.VMEM((pairs,) + rows, kind),
            pltpu.VMEM((pairs,) + chunks, kind),
            pltpu.VMEM((pairs,) + rows, kind),
            pltpu.VMEM((pairs,) + chunks, kind),
            pltpu.VMEM((pairs,) + rows, kind),
            pltpu.VMEM(chunks, kind),
            dma(many),
            dma(many),
            dma(many),
            dma(many),
            dma((ep_count,)),
            dma((ep_count,)),
        ],
        compiler_params=pltpu.CompilerParams(collective_id=1, has_side_effects=True),
    )(parts, mix)


def span_recurrence(query, inflow, decay_logarithm, values):
    number_of_heads, seq_len, key_width = query.shape
    span_count = seq_len // SPAN

    def to_spans(array):
        return array.reshape(number_of_heads, span_count, SPAN, array.shape[-1]).transpose(
            1, 0, 2, 3
        )

    lower_mask = jnp.tril(jnp.ones((SPAN, SPAN), bool))

    def advance(carried, inputs):
        query_span, inflow_span, decay_span, value_span = inputs
        running = jnp.cumsum(decay_span, axis=1)
        lifted_query = query_span * jnp.exp(running)
        lowered_inflow = inflow_span * jnp.exp(-running)
        scores = jnp.einsum("htd,hsd->hts", lifted_query, lowered_inflow, precision=highest)
        scores = jnp.where(lower_mask[None, :, :], scores, 0.0)
        output = jnp.einsum("hts,hsv->htv", scores, value_span, precision=highest)
        output = output + jnp.einsum("htd,hdv->htv", lifted_query, carried, precision=highest)
        closing = running[:, -1:, :]
        updated = jnp.exp(closing[:, 0, :])[:, :, None] * carried + jnp.einsum(
            "hsd,hsv->hdv", inflow_span * jnp.exp(closing - running), value_span, precision=highest
        )
        return (updated, output)

    start_state = jnp.zeros((number_of_heads, key_width, values.shape[-1]), jnp.float32)
    final_state, outputs = lax.scan(
        advance,
        start_state,
        (to_spans(query), to_spans(inflow), to_spans(decay_logarithm), to_spans(values)),
        unroll=True,
    )
    return (
        final_state,
        outputs.transpose(1, 0, 2, 3).reshape(number_of_heads, seq_len, values.shape[-1]),
    )


def slot_positions(block_routes, expert_count):
    chosen = block_routes.reshape(-1)
    table = (chosen[:, None] == jnp.arange(expert_count, dtype=jnp.int32)[None, :]).astype(
        jnp.int32
    )
    before = jnp.cumsum(table, axis=0) - table
    return (chosen, jnp.sum(before * table, axis=1))


def expert_hidden(flat_rows, gate_local, up_local):
    gate_proj = jnp.dot(flat_rows, gate_local, preferred_element_type=jnp.float32)
    up_proj = jnp.dot(flat_rows, up_local, preferred_element_type=jnp.float32)
    return (jax.nn.silu(gate_proj) * up_proj).astype(jnp.bfloat16)


def per_device(
    recurrence_query,
    forget_preactivation,
    recurrence_value,
    output_gate_preactivation,
    forget_margin,
    surge_log_decay,
    head_norm_gain,
    recurrence_output_matrix,
    second_micro_input,
    expert_norm_gain,
    routes,
    router_chosen_logits,
    expert_gate_matrix,
    expert_up_matrix,
    expert_down_matrix,
):
    number_of_heads = surge_log_decay.shape[0]
    seq_len = recurrence_query.shape[0]

    def heads_leading(array):
        return array.astype(jnp.float32).reshape(seq_len, number_of_heads, -1).transpose(1, 0, 2)

    closed_flag = jax.nn.sigmoid(-forget_preactivation.astype(jnp.float32)) * forget_margin
    decay_logarithm = heads_leading(jnp.log1p(-closed_flag)) + surge_log_decay[:, :, None]
    query = heads_leading(recurrence_query)
    final_state, local_out = span_recurrence(
        query, heads_leading(closed_flag), decay_logarithm, heads_leading(recurrence_value)
    )
    running = jnp.cumsum(decay_logarithm, axis=1)
    totals = running[:, -1, :]
    tp_count = lax.axis_size("tp")
    tp_rank = lax.axis_index("tp")
    ep_rank = lax.axis_index("ep")
    expert_count = lax.axis_size("ep")
    tok_rows = second_micro_input.shape[0]
    width = second_micro_input.shape[1]
    capacity = 2 * tok_rows * TOP // expert_count
    moe_rows = second_micro_input.astype(jnp.float32)
    normed = (
        moe_rows
        * lax.rsqrt(jnp.mean(moe_rows * moe_rows, axis=-1, keepdims=True) + epsilon)
        * expert_norm_gain
    ).astype(jnp.bfloat16)
    own_routes = lax.dynamic_slice_in_dim(routes, tp_rank * tok_rows, tok_rows, 0)
    own_chosen, own_places = slot_positions(own_routes, expert_count)
    spot = (own_chosen * capacity + own_places).reshape(tok_rows, TOP)
    numbers = jnp.arange(expert_count * capacity, dtype=jnp.int32)
    taken = spot[:, :, None] == numbers
    chooser = jnp.sum(taken.astype(jnp.bfloat16), axis=1)
    slots = jnp.dot(chooser.T, normed, preferred_element_type=jnp.float32).astype(jnp.bfloat16)
    slots = slots.reshape(expert_count, capacity, width)
    coarse = totals.astype(jnp.bfloat16)
    fine = (totals - coarse.astype(jnp.float32)).astype(jnp.bfloat16)
    packed = jnp.concatenate(
        [
            final_state.astype(jnp.bfloat16),
            jnp.swapaxes(jnp.stack([coarse, fine], axis=-1), 1, 2),
        ],
        axis=1,
    )
    piece, states = dispatch(slots, packed, expert_count, tp_count)
    key_rows = final_state.shape[1]
    ranks = jnp.arange(expert_count)
    all_totals = jnp.sum(states[:, :, key_rows:, :].astype(jnp.float32), axis=2)
    between = (ranks[None, :] > ranks[:, None]) & (ranks[None, :] < ep_rank)
    spans_after = jnp.sum(jnp.where(between[:, :, None, None], all_totals[None], 0.0), axis=1)
    survive = jnp.where((ranks < ep_rank)[:, None, None], jnp.exp(spans_after), 0.0)
    entering = jnp.sum(
        survive[:, :, :, None] * states[:, :, :key_rows, :].astype(jnp.float32), axis=0
    )
    output = local_out + jnp.einsum(
        "htd,hdv->htv", query * jnp.exp(running), entering, precision=highest
    )
    output = output * lax.rsqrt(jnp.mean(output * output, axis=-1, keepdims=True) + epsilon)
    output = output.transpose(1, 0, 2).reshape(seq_len, -1)
    hidden_a = (
        output * head_norm_gain * jax.nn.silu(output_gate_preactivation.astype(jnp.float32))
    ).astype(jnp.bfloat16)
    hidden_b = expert_hidden(
        piece.reshape(-1, width), expert_gate_matrix[0], expert_up_matrix[0]
    )
    mix_rows = seq_len // tp_count
    mix_parts = jnp.dot(
        hidden_a, recurrence_output_matrix, preferred_element_type=jnp.float32
    ).astype(jnp.bfloat16)
    expert_parts = jnp.dot(
        hidden_b, expert_down_matrix[0], preferred_element_type=jnp.float32
    ).astype(jnp.bfloat16)
    mixed, returned = give_back(
        expert_parts.reshape(piece.shape),
        mix_parts.reshape(tp_count, mix_rows, width),
        expert_count,
        tp_count,
    )
    route_weight = jax.nn.softmax(router_chosen_logits, axis=-1)
    weights = jnp.sum(jnp.where(taken, route_weight[:, :, None], 0.0), axis=1)
    moe_out = jnp.dot(
        weights, returned.reshape(-1, width).astype(jnp.float32), precision=highest
    )
    return (mixed, moe_out.astype(jnp.bfloat16))


def solution(mesh):
    return jax.shard_map(
        per_device,
        mesh=mesh,
        in_specs=(
            P("ep", "tp"),
            P("ep", "tp"),
            P("ep", "tp"),
            P("ep", "tp"),
            P("tp"),
            P("tp", "ep"),
            P("tp"),
            P("tp", None),
            P(("ep", "tp"), None),
            P(),
            P("ep", None),
            P(("ep", "tp"), None),
            P("ep", None, "tp"),
            P("ep", None, "tp"),
            P("ep", "tp", None),
        ),
        out_specs=(P(("ep", "tp"), None), P(("ep", "tp"), None)),
        check_vma=False,
    )
```

```python
import functools

import jax
import jax.numpy as jnp
from jax import lax
from jax.experimental import pallas as pl
from jax.experimental.pallas import tpu as pltpu
from jax.sharding import PartitionSpec as P

TOP = 2
SPAN = 64
MESH = pl.DeviceIdType.MESH


epsilon = 1e-06
highest = lax.Precision.HIGHEST


def visiting_order(count):
    return sorted(range(1, count), key=lambda k: abs(k - count // 2)) + [0]


def greet(me, tp, ep_count, tp_count, wait=True):
    pairs = tp_count // 2
    pair, side = tp // 2, tp % 2
    barrier = pltpu.get_barrier_semaphore()
    for k in range(1, ep_count):
        pl.semaphore_signal(
            barrier,
            inc=1,
            device_id={"ep": lax.rem(me + k, ep_count), "tp": tp},
            device_id_type=MESH,
        )
    for j in range(1, pairs):
        pl.semaphore_signal(
            barrier,
            inc=1,
            device_id={"ep": me, "tp": lax.rem(pair + j, pairs) * 2 + side},
            device_id_type=MESH,
        )
    pl.semaphore_signal(
        barrier, inc=1, device_id={"ep": me, "tp": pair * 2 + 1 - side}, device_id_type=MESH
    )
    if wait:
        pl.semaphore_wait(barrier, ep_count + pairs - 1)


def product(left, right, left_axis, right_axis, precision=None):
    return lax.dot_general(
        left,
        right,
        (((left_axis,), (right_axis,)), ((), ())),
        precision=precision,
        preferred_element_type=jnp.float32,
    )


def iota(shape, axis):
    return lax.broadcasted_iota(jnp.int32, shape, axis)


def dispatch_kernel(
    ep_count,
    tp_count,
    query_ref,
    forget_ref,
    value_ref,
    opening_ref,
    margin_ref,
    surge_ref,
    head_gain_ref,
    tokens_ref,
    gain_ref,
    routes_ref,
    logits_ref,
    gate_hbm,
    up_hbm,
    hidden_b_ref,
    hidden_a_ref,
    weights_ref,
    slots,
    piece,
    gate,
    up,
    lifted_ref,
    local_ref,
    window,
    window_total,
    before,
    before_total,
    outgoing,
    incoming,
    load,
    sa,
    ra,
    sy,
    ry,
    sc,
    rc,
    ss,
    rs,
):
    wide = jnp.float32
    me, tp = lax.axis_index("ep"), lax.axis_index("tp")
    pairs = tp_count // 2
    pair, side = tp // 2, tp % 2
    other = pair * 2 + 1 - side
    order = visiting_order(ep_count)
    heads, seq_len = surge_ref.shape
    key_width = query_ref.shape[1] // heads
    value_width = value_ref.shape[1] // heads
    tok_rows = tokens_ref.shape[0]
    capacity = slots.shape[1]
    slot_count = ep_count * capacity
    steps = outgoing.shape[0]

    greet(me, tp, ep_count, tp_count, wait=False)
    fetch = [
        pltpu.make_async_copy(gate_hbm, gate, load.at[0]),
        pltpu.make_async_copy(up_hbm, up, load.at[1]),
    ]
    for copy in fetch:
        copy.start()

    def remote(src, dst, send, recv, ep, to):
        return pltpu.make_async_remote_copy(
            src_ref=src,
            dst_ref=dst,
            send_sem=send,
            recv_sem=recv,
            device_id={"ep": ep, "tp": to},
            device_id_type=MESH,
        )

    def exchange(k):
        to = lax.rem(me + k, ep_count)
        return remote(slots.at[to], piece.at[tp, me], sa.at[k], ra.at[k], to, tp)

    def source(k):
        return lax.rem(me + ep_count - k, ep_count)

    def own_block(k):
        return slots.at[me] if k == 0 else piece.at[tp, source(k)]

    def across(k, j):
        to = lax.rem(pair + j, pairs) * 2 + side
        return remote(own_block(k), piece.at[tp, source(k)], sy.at[j, k], ry.at[j, k], me, to)

    def beside(k, j):
        block = lax.rem(pair + pairs - j, pairs) * 2 + side
        src = own_block(k) if j == 0 else piece.at[block, source(k)]
        return remote(src, piece.at[block, source(k)], sc.at[j, k], rc.at[j, k], me, other)

    def pass_on(k):
        for j in range(1, pairs):
            across(k, j).start()
        beside(k, 0).start()

    rows = tokens_ref[...].astype(wide)
    normed = (
        rows * lax.rsqrt(jnp.mean(rows * rows, axis=-1, keepdims=True) + epsilon) * gain_ref[...]
    ).astype(jnp.bfloat16)
    routes = routes_ref[pl.ds(pl.multiple_of(tp * tok_rows, tok_rows), tok_rows), :]
    named = [routes[:, i : i + 1] for i in range(TOP)]
    experts = iota((tok_rows, ep_count), 1)
    tables = [(column == experts).astype(wide) for column in named]
    strict = (iota((tok_rows, tok_rows), 0) > iota((tok_rows, tok_rows), 1)).astype(wide)
    earlier = product(strict, sum(tables), 1, 0, highest)
    places = [jnp.sum(earlier * table, axis=1, keepdims=True) for table in tables]
    spots = [
        column * capacity + place.astype(jnp.int32) for column, place in zip(named, places)
    ]
    for number, k in enumerate(order):
        to = lax.rem(me + k, ep_count)
        wanted = iota((tok_rows, capacity), 1) + to * capacity
        chooser = sum((spot == wanted).astype(wide) for spot in spots).astype(jnp.bfloat16)
        slots[to] = product(chooser, normed, 0, 0).astype(jnp.bfloat16)
        if number == 0:
            pl.semaphore_wait(pltpu.get_barrier_semaphore(), ep_count + pairs - 1)
        if k:
            exchange(k).start()
    pass_on(0)
    piece[tp, me] = slots[me]

    at, since = iota((seq_len, seq_len), 0), iota((seq_len, seq_len), 1)
    shut = jax.nn.sigmoid(-forget_ref[...].astype(wide)) * margin_ref[...]
    logarithm = jnp.log1p(-shut)
    within = ((at >= since) & (at // SPAN == since // SPAN)).astype(wide)
    running_all = product(within, logarithm, 1, 0, highest)
    triangle = iota((SPAN, SPAN), 0) >= iota((SPAN, SPAN), 1)
    for head in range(heads):
        keys = slice(head * key_width, (head + 1) * key_width)
        values = slice(head * value_width, (head + 1) * value_width)
        surges = jnp.sum(within * surge_ref[head : head + 1, :], axis=1, keepdims=True)
        running_head = running_all[:, keys] + surges
        state = jnp.zeros((value_width, key_width), wide)
        total = jnp.zeros((1, key_width), wide)
        for span in range(seq_len // SPAN):
            part = slice(span * SPAN, (span + 1) * SPAN)
            running = running_head[part]
            closing = running[SPAN - 1 : SPAN]
            inflow = shut[part, keys]
            value = value_ref[part, values].astype(wide)
            query = query_ref[part, keys].astype(wide)
            lifted = query * jnp.exp(running)
            scores = product(lifted, inflow * jnp.exp(-running), 1, 1, highest)
            scores = jnp.where(triangle, scores, 0.0)
            local = product(scores, value, 1, 0, highest)
            if span:
                local = local + product(lifted, state, 1, 1, highest)
            local_ref[part, values] = local
            lifted_ref[part, keys] = query * jnp.exp(running + total)
            fresh = product(value, inflow * jnp.exp(closing - running), 0, 0, highest)
            state = jnp.exp(closing) * state + fresh
            total = total + closing
        window[head] = state
        window_total[head] = total
    before[...] = jnp.zeros_like(before)
    before_total[...] = jnp.zeros_like(before_total)

    def state_copy(step):
        to = lax.rem(me + 2**step, ep_count)
        return remote(outgoing.at[step], incoming.at[step], ss.at[step], rs.at[step], to, tp)

    def send_window(step):
        for head in range(heads):
            outgoing[step, head, :value_width] = window[head].astype(jnp.bfloat16)
            total = window_total[head]
            coarse = total.astype(jnp.bfloat16).astype(wide)
            line = iota((16, key_width), 0)
            tail = jnp.where(line == 0, coarse, jnp.where(line == 1, total - coarse, 0.0))
            outgoing[step, head, value_width:] = tail.astype(jnp.bfloat16)

        @pl.when(me + 2**step < ep_count)
        def _():
            state_copy(step).start()

    def take_window(step):
        @pl.when(me >= 2**step)
        def _():
            state_copy(step).wait_recv()
            for head in range(heads):
                state = incoming[step, head, :value_width].astype(wide)
                total = jnp.sum(
                    incoming[step, head, value_width:].astype(wide), axis=0, keepdims=True
                )
                before[head] = jnp.exp(before_total[head]) * state + before[head]
                before_total[head] = before_total[head] + total
                window[head] = jnp.exp(window_total[head]) * state + window[head]
                window_total[head] = window_total[head] + total

    sequence = [0] + order[:-1]
    done = 0
    send_window(0)
    for position, k in enumerate(sequence):
        if k:
            exchange(k).wait_recv()
            pass_on(k)
        if position:
            last = sequence[position - 1]
            for j in range(1, pairs):
                across(last, j).wait_recv()
                beside(last, j).start()
        if position >= 2 and position % 2 == 0 and done < steps:
            take_window(done)
            done += 1
            if done < steps:
                send_window(done)
    while done < steps:
        take_window(done)
        done += 1
        if done < steps:
            send_window(done)
    for j in range(1, pairs):
        across(sequence[-1], j).wait_recv()
        beside(sequence[-1], j).start()

    for head in range(heads):
        keys = slice(head * key_width, (head + 1) * key_width)
        values = slice(head * value_width, (head + 1) * value_width)
        out = local_ref[:, values] + product(lifted_ref[:, keys], before[head], 1, 1, highest)
        out = out * lax.rsqrt(jnp.mean(out * out, axis=-1, keepdims=True) + epsilon)
        opening = opening_ref[:, values].astype(wide)
        hidden_a_ref[:, values] = (
            out * head_gain_ref[:, values] * (opening * jax.nn.sigmoid(opening))
        ).astype(jnp.bfloat16)
    logits = logits_ref[...]
    raised = jnp.exp(logits - jnp.max(logits, axis=-1, keepdims=True))
    share = raised / jnp.sum(raised, axis=-1, keepdims=True)
    numbers = iota((tok_rows, slot_count), 1)
    weights_ref[...] = sum(
        jnp.where(spot == numbers, share[:, i : i + 1], 0.0) for i, spot in enumerate(spots)
    )

    for k in sequence:
        for j in range(pairs):
            beside(k, j).wait_recv()
    for copy in fetch:
        copy.wait()

    def experts_of(block, carry):
        if capacity % 16:
            taken = jnp.concatenate([piece[block, e] for e in range(ep_count)], axis=0)
        else:
            taken = piece[block].reshape(slot_count, piece.shape[-1])
        left = product(taken, gate[...], 1, 0)
        right = product(taken, up[...], 1, 0)
        hidden_b_ref[block] = (left * jax.nn.sigmoid(left) * right).astype(jnp.bfloat16)
        return carry

    lax.fori_loop(0, tp_count, experts_of, 0)

    for k in range(1, ep_count):
        exchange(k).wait_send()
    for k in sequence:
        for j in range(pairs):
            if j:
                across(k, j).wait_send()
            beside(k, j).wait_send()
    for step in range(steps):

        @pl.when(me + 2**step < ep_count)
        def _(step=step):
            state_copy(step).wait_send()


def dispatch(small, gate, up, heads, capacity, ep_count, tp_count):
    pairs = tp_count // 2
    dma = pltpu.SemaphoreType.DMA
    vmem = pl.BlockSpec(memory_space=pltpu.VMEM)
    hbm = pl.BlockSpec(memory_space=pl.ANY)
    query, value, tokens = small[0], small[2], small[7]
    seq_len, keys = query.shape
    values = value.shape[1]
    tok_rows, width = tokens.shape
    key_width, value_width = keys // heads, values // heads
    steps = (ep_count - 1).bit_length()
    both = dma((pairs, ep_count))
    kind = jnp.bfloat16
    return pl.pallas_call(
        functools.partial(dispatch_kernel, ep_count, tp_count),
        out_shape=(
            jax.ShapeDtypeStruct((tp_count, ep_count * capacity, gate.shape[1]), kind),
            jax.ShapeDtypeStruct((seq_len, values), kind),
            jax.ShapeDtypeStruct((tok_rows, ep_count * capacity), jnp.float32),
        ),
        in_specs=[vmem] * len(small) + [hbm] * 2,
        out_specs=(vmem, vmem, vmem),
        scratch_shapes=[
            pltpu.VMEM((ep_count, capacity, width), kind),
            pltpu.VMEM((tp_count, ep_count, capacity, width), kind),
            pltpu.VMEM(gate.shape, kind),
            pltpu.VMEM(up.shape, kind),
            pltpu.VMEM((seq_len, keys), jnp.float32),
            pltpu.VMEM((seq_len, values), jnp.float32),
            pltpu.VMEM((heads, value_width, key_width), jnp.float32),
            pltpu.VMEM((heads, 1, key_width), jnp.float32),
            pltpu.VMEM((heads, value_width, key_width), jnp.float32),
            pltpu.VMEM((heads, 1, key_width), jnp.float32),
            pltpu.VMEM((steps, heads, value_width + 16, key_width), kind),
            pltpu.VMEM((steps, heads, value_width + 16, key_width), kind),
            dma((2,)),
            dma((ep_count,)),
            dma((ep_count,)),
            both,
            both,
            both,
            both,
            dma((steps,)),
            dma((steps,)),
        ],
        compiler_params=pltpu.CompilerParams(
            collective_id=0, has_side_effects=True, vmem_limit_bytes=60 << 20
        ),
    )(*small, gate, up)


def return_kernel(
    ep_count,
    tp_count,
    parts,
    mix,
    mixed,
    returned,
    cbuf,
    cmix,
    ysend,
    ysmix,
    ybuf,
    ymix,
    abuf,
    sc,
    rc,
    sy,
    ry,
    sa,
    ra,
):
    me, tp = lax.axis_index("ep"), lax.axis_index("tp")
    pairs = tp_count // 2
    pair, side = tp // 2, tp % 2
    other = pair * 2 + 1 - side
    order = visiting_order(ep_count)
    greet(me, tp, ep_count, tp_count)

    def remote(src, dst, send, recv, ep, to):
        return pltpu.make_async_remote_copy(
            src_ref=src,
            dst_ref=dst,
            send_sem=send,
            recv_sem=recv,
            device_id={"ep": ep, "tp": to},
            device_id_type=MESH,
        )

    def chunk(k):
        return lax.rem(me + k, ep_count)

    def toward(j):
        return lax.rem(pair + j, pairs)

    def beside(k, j):
        block = toward(j) * 2 + 1 - side
        if k == ep_count:
            return remote(mix.at[block], cmix.at[j], sc.at[j, k], rc.at[j, k], me, other)
        return remote(parts.at[block, chunk(k)], cbuf.at[j, k], sc.at[j, k], rc.at[j, k], me, other)

    def across(k, j):
        to = toward(j) * 2 + side
        if k == ep_count:
            return remote(ysmix.at[j], ymix.at[j], sy.at[j, k], ry.at[j, k], me, to)
        return remote(ysend.at[j, k], ybuf.at[j, k], sy.at[j, k], ry.at[j, k], me, to)

    def home(k):
        return remote(abuf.at[k], returned.at[me], sa.at[k], ra.at[k], chunk(k), tp)

    wide = jnp.float32
    everything = order + [ep_count]
    for k in everything:
        for j in list(range(1, pairs)) + [0]:
            beside(k, j).start()
    for k in everything:
        for j in range(1, pairs):
            beside(k, j).wait_recv()
            block = toward(j) * 2 + side
            if k == ep_count:
                ysmix[j] = (mix[block].astype(wide) + cmix[j].astype(wide)).astype(mix.dtype)
            else:
                ysend[j, k] = (
                    parts[block, chunk(k)].astype(wide) + cbuf[j, k].astype(wide)
                ).astype(parts.dtype)
            across(k, j).start()
    for k in everything:
        beside(k, 0).wait_recv()
        if k == ep_count:
            total = mix[tp].astype(wide) + cmix[0].astype(wide)
        else:
            total = parts[tp, chunk(k)].astype(wide) + cbuf[0, k].astype(wide)
        for j in range(1, pairs):
            across(k, j).wait_recv()
            total = total + (ymix[j] if k == ep_count else ybuf[j, k]).astype(wide)
        total = total.astype(parts.dtype)
        if k == ep_count:
            mixed[...] = total
        elif k == 0:
            returned[me] = total
        else:
            abuf[k] = total
            home(k).start()
    for k in everything:
        for j in range(pairs):
            beside(k, j).wait_send()
            if j:
                across(k, j).wait_send()
        if 0 < k < ep_count:
            home(k).wait()


def give_back(parts, mix, ep_count, tp_count):
    pairs = tp_count // 2
    dma = pltpu.SemaphoreType.DMA
    vmem = pl.BlockSpec(memory_space=pltpu.VMEM)
    chunks, rows = parts.shape[1:], mix.shape[1:]
    many = (pairs, ep_count + 1)
    kind = parts.dtype
    return pl.pallas_call(
        functools.partial(return_kernel, ep_count, tp_count),
        out_shape=(
            jax.ShapeDtypeStruct(rows, kind),
            jax.ShapeDtypeStruct(chunks, kind),
        ),
        in_specs=[vmem] * 2,
        out_specs=(vmem, vmem),
        scratch_shapes=[
            pltpu.VMEM((pairs,) + chunks, kind),
            pltpu.VMEM((pairs,) + rows, kind),
            pltpu.VMEM((pairs,) + chunks, kind),
            pltpu.VMEM((pairs,) + rows, kind),
            pltpu.VMEM((pairs,) + chunks, kind),
            pltpu.VMEM((pairs,) + rows, kind),
            pltpu.VMEM(chunks, kind),
            dma(many),
            dma(many),
            dma(many),
            dma(many),
            dma((ep_count,)),
            dma((ep_count,)),
        ],
        compiler_params=pltpu.CompilerParams(collective_id=1, has_side_effects=True),
    )(parts, mix)


def per_device(
    recurrence_query,
    forget_preactivation,
    recurrence_value,
    output_gate_preactivation,
    forget_margin,
    surge_log_decay,
    head_norm_gain,
    recurrence_output_matrix,
    second_micro_input,
    expert_norm_gain,
    routes,
    router_chosen_logits,
    expert_gate_matrix,
    expert_up_matrix,
    expert_down_matrix,
):
    number_of_heads = surge_log_decay.shape[0]
    seq_len = recurrence_query.shape[0]
    tp_count = lax.axis_size("tp")
    expert_count = lax.axis_size("ep")
    tok_rows, width = second_micro_input.shape
    capacity = 2 * tok_rows * TOP // expert_count
    small = (
        recurrence_query,
        forget_preactivation,
        recurrence_value,
        output_gate_preactivation,
        forget_margin[None, :],
        surge_log_decay,
        head_norm_gain[None, :],
        second_micro_input,
        expert_norm_gain[None, :],
        routes,
        router_chosen_logits,
    )
    hidden_b, hidden_a, weights = dispatch(
        small,
        expert_gate_matrix[0],
        expert_up_matrix[0],
        number_of_heads,
        capacity,
        expert_count,
        tp_count,
    )
    hidden_b = hidden_b.reshape(-1, hidden_b.shape[-1])
    mix_rows = seq_len // tp_count
    mix_parts = jnp.dot(
        hidden_a, recurrence_output_matrix, preferred_element_type=jnp.float32
    ).astype(jnp.bfloat16)
    expert_parts = jnp.dot(
        hidden_b, expert_down_matrix[0], preferred_element_type=jnp.float32
    ).astype(jnp.bfloat16)
    mixed, returned = give_back(
        expert_parts.reshape(tp_count, expert_count, capacity, width),
        mix_parts.reshape(tp_count, mix_rows, width),
        expert_count,
        tp_count,
    )
    moe_out = jnp.dot(
        weights, returned.reshape(-1, width).astype(jnp.float32), precision=highest
    )
    return (mixed, moe_out.astype(jnp.bfloat16))


def solution(mesh):
    return jax.shard_map(
        per_device,
        mesh=mesh,
        in_specs=(
            P("ep", "tp"),
            P("ep", "tp"),
            P("ep", "tp"),
            P("ep", "tp"),
            P("tp"),
            P("tp", "ep"),
            P("tp"),
            P("tp", None),
            P(("ep", "tp"), None),
            P(),
            P("ep", None),
            P(("ep", "tp"), None),
            P("ep", None, "tp"),
            P("ep", None, "tp"),
            P("ep", "tp", None),
        ),
        out_specs=(P(("ep", "tp"), None), P(("ep", "tp"), None)),
        check_vma=False,
    )
```
